32 devices in a mesh: kv: 8 (over z, x), tp: 4 (over y, core).
Axes of the slice: x: 2, y: 2, z: 4, core: 2. Of those that a mesh axis runs over, the one named last changes fastest.
Arguments:
- hidden: bfloat16 [128, 4, 2048], P(None, None, 'kv'), may hold values from -18 to 18
- norm_gain: float32 [2048], replicated, may hold values from 0.1 to 1.9
- w_query: bfloat16 [2048, 1024], P(None, 'tp'), may hold values from -0.125 to 0.125
- w_forget: bfloat16 [2048, 1024], P(None, 'tp'), may hold values from -0.125 to 0.125
- w_input: bfloat16 [2048, 1024], P(None, 'tp'), may hold values from -0.125 to 0.125
- w_outgate: bfloat16 [2048, 1024], P(None, 'tp'), may hold values from -0.125 to 0.125
- w_out: bfloat16 [1024, 2048], replicated, may hold values from -0.1875 to 0.1875
- floor: float32 [1024], P('tp'), may hold values from 0 to 0.95
- head_gain: float32 [128], replicated, may hold values from 0.1 to 1.9
- base_state: float32 [128, 8, 128, 128], P('kv', 'tp'), may hold values from -4 to 4
- prev_forget: bfloat16 [128, 4, 1024], P('kv', None, 'tp'), may hold values from -6 to 6
- prev_input: bfloat16 [128, 4, 1024], P('kv', None, 'tp'), may hold values from -6 to 6
- accepted: int32 [128], P('kv'), may hold values from 0 to 4
Outputs:
- mixed: bfloat16 [128, 4, 2048], P(None, None, 'kv')
- taken_state: float32 [128, 8, 128, 128], P('kv', 'tp')
The draws below stay inside these ranges and needn't reach their ends.
All inputs are finite; a program needn't handle non-finite values.
Results may differ from the reference program's by a relative error of at most 0.014.
Values may be sent and summed in bfloat16 or wider, within the bound.
No kernel may reach another device: no remote copies, remote signals or barrier semaphores. Data moves between devices by JAX's collectives and lax.ppermute only.
A program may use at most 64 MiB of HBM per device.

```python
import jax
import jax.numpy as jnp
from jax import lax

D = 2048
HEADS = 8
HEAD_DIM = 128
PROPS = 4
SEQ_DEV = 16
WIDTH = 1024
SEQS = 128
N_KV = 8


def draw_hidden(key, part):
    columns = jnp.arange(D, dtype=jnp.float32) / D
    base = jnp.clip(jax.random.normal(key, (SEQ_DEV * N_KV, PROPS, D), jnp.float32), -6.0, 6.0)
    return (base * 3.0 ** columns).astype(jnp.bfloat16)


def touch_ends(entries, stream_key, smallest, top_value):
    longest = entries.shape.index(max(entries.shape))
    spots = []
    for shift in (0, 1):
        where = [jax.random.randint(jax.random.fold_in(stream_key, axis), (), 0, length) for axis, length in enumerate(entries.shape)]
        where[longest] = (where[longest] + shift) % entries.shape[longest]
        spots.append(tuple(where))
    return entries.at[spots[0]].set(smallest).at[spots[1]].set(top_value)


def levels(stream_key, shape, pieces, least, high):
    def one(dim, parts):
        steps = jax.random.uniform(jax.random.fold_in(jax.random.fold_in(stream_key, 6), dim), (parts,), jnp.float32, least / len(pieces), high / len(pieces))
        return jnp.repeat(jnp.exp(steps), shape[dim] // parts).reshape((-1,) + (1,) * (len(shape) - dim - 1))

    loudness = one(*pieces[0])
    for cut in pieces[1:]:
        loudness = loudness * one(*cut)
    return loudness


def centred(key, extent, width, reach, cuts=(), held_as=jnp.bfloat16):
    loudness = levels(key, extent, cuts, -0.22, 0.18) if cuts else 1.0
    values = jax.random.normal(key, extent, jnp.float32) * width * loudness
    return jnp.minimum(jnp.maximum(values, -reach), reach).astype(held_as)


def setup_inputs(seed: int = 0) -> dict:
    splits = jax.random.split(jax.random.key(seed), 14)
    hidden = draw_hidden(jax.random.fold_in(splits[13], 71), 0)
    norm_gain = jnp.clip(1.0 + 0.18 * jax.random.normal(splits[1], (D,), jnp.float32), 0.1, 1.9)
    w_query = centred(splits[2], (D, WIDTH), D ** -0.5, 0.125, ((1, 4),))
    w_forget = centred(splits[3], (D, WIDTH), D ** -0.5, 0.125, ((1, 4),))
    w_input = centred(splits[4], (D, WIDTH), D ** -0.5, 0.125, ((1, 4),))
    w_outgate = centred(splits[5], (D, WIDTH), D ** -0.5, 0.125, ((1, 4),))
    w_out = centred(splits[6], (WIDTH, D), WIDTH ** -0.5, 0.1875)
    floor = jnp.clip(0.95 * jax.random.uniform(splits[7], (WIDTH,), jnp.float32) ** levels(splits[7], (WIDTH,), ((0, 4),), -0.2, 0.2), 0.0, 0.95)
    head_gain = jnp.clip(1.0 + 0.18 * jax.random.normal(splits[8], (HEAD_DIM,), jnp.float32), 0.1, 1.9)
    base_state = centred(splits[9], (SEQS, HEADS, HEAD_DIM, HEAD_DIM), 0.3, 4.0, ((0, 8), (1, 4)), jnp.float32)
    prev_forget = centred(splits[10], (SEQS, PROPS, WIDTH), 1.5, 6.0, ((0, 8), (2, 4)))
    prev_input = centred(splits[11], (SEQS, PROPS, WIDTH), 1.0, 6.0, ((0, 8), (2, 4)))
    accepted = touch_ends(jax.random.randint(splits[12], (SEQS,), 0, PROPS + 1), jax.random.fold_in(splits[12], 1), 0, PROPS).astype(jnp.int32)
    return {"hidden": hidden, "norm_gain": norm_gain, "w_query": w_query, "w_forget": w_forget, "w_input": w_input, "w_outgate": w_outgate, "w_out": w_out, "floor": floor, "head_gain": head_gain, "base_state": base_state, "prev_forget": prev_forget, "prev_input": prev_input, "accepted": accepted}


def reference(hidden, norm_gain, w_query, w_forget, w_input, w_outgate, w_out, floor, head_gain, base_state, prev_forget, prev_input, accepted):
    values_in = hidden.astype(jnp.float32)
    squares = lax.optimization_barrier(jnp.sum(values_in * values_in, axis=2))
    normed = (values_in * lax.rsqrt(squares / D + 1e-06)[..., None] * norm_gain).astype(jnp.bfloat16)
    query_pre = jnp.dot(normed, w_query, preferred_element_type=jnp.float32).astype(jnp.bfloat16)
    forget_pre = jnp.dot(normed, w_forget, preferred_element_type=jnp.float32).astype(jnp.bfloat16)
    input_pre = jnp.dot(normed, w_input, preferred_element_type=jnp.float32).astype(jnp.bfloat16)
    gate_pre = jnp.dot(normed, w_outgate, preferred_element_type=jnp.float32).astype(jnp.bfloat16)
    seqs = hidden.shape[0]
    shape = (seqs, PROPS, HEADS, HEAD_DIM)
    query = jax.nn.silu(query_pre.astype(jnp.float32)).reshape(shape)
    forget = (floor + (1.0 - floor) * jax.nn.sigmoid(forget_pre.astype(jnp.float32))).reshape(shape)
    value = input_pre.astype(jnp.float32).reshape(shape)
    prev_f = (floor + (1.0 - floor) * jax.nn.sigmoid(prev_forget.astype(jnp.float32))).reshape(shape)
    prev_v = prev_input.astype(jnp.float32).reshape(shape)
    state = base_state
    for step in range(PROPS):
        live = (step < accepted)[:, None, None, None]
        moved = prev_f[:, step][..., None] * state + (1.0 - prev_f[:, step])[..., None] * prev_v[:, step][:, :, None, :]
        state = jnp.where(live, moved, state)
    taken_state = state
    outputs = []
    for step in range(PROPS):
        state = forget[:, step][..., None] * state + (1.0 - forget[:, step])[..., None] * value[:, step][:, :, None, :]
        outputs.append(jnp.einsum('bhk,bhkv->bhv', query[:, step], state, precision=lax.Precision.HIGHEST))
    result = jnp.stack(outputs, axis=1)
    scaled = result * lax.rsqrt(lax.optimization_barrier(jnp.mean(result * result, axis=-1, keepdims=True)) + 1e-05) * head_gain
    gated = scaled * jax.nn.silu(gate_pre.astype(jnp.float32)).reshape(shape)
    mixed_heads = gated.reshape(seqs, PROPS, HEADS * HEAD_DIM).astype(jnp.bfloat16)
    mixed = jnp.dot(mixed_heads, w_out, preferred_element_type=jnp.float32).astype(jnp.bfloat16)
    return (mixed, taken_state)
```

```python
import functools

import jax
import jax.numpy as jnp
from jax import lax
from jax.experimental import pallas as pl
from jax.experimental.pallas import tpu as pltpu
from jax.sharding import PartitionSpec as P

HEAD_DIM = 128
F32 = jnp.float32
BF16 = jnp.bfloat16


def exchange(blocks, n_kv, n_tp):
    r = n_kv // n_tp
    kv = lax.axis_index("kv")
    got = []
    for j in range(r):
        perm = []
        for k in range(n_kv):
            for s in range(n_tp):
                to_kv = r * s + (j + k) % r
                perm.append((k * n_tp + s, to_kv * n_tp + k // r))
        if r == 2:
            sent = jnp.where((kv + j) % r == 0, blocks[0], blocks[1])
        else:
            sent = lax.dynamic_index_in_dim(blocks, (kv + j) % r, 0, keepdims=False)
        got.append(lax.ppermute(sent, ("kv", "tp"), perm))
    if r == 2:
        even = kv % r == 0
        mine = jnp.stack([jnp.where(even, got[0], got[1]), jnp.where(even, got[1], got[0])])
    else:
        mine = jnp.take(jnp.stack(got), (kv - jnp.arange(r)) % r, axis=0)
    return mine


def state_kernel(seqs, props, heads, acc, floor, prev_forget, prev_input, base, taken, low, a_sc, b_sc, s_sc, in_sem, out_sem):
    loads = [pltpu.make_async_copy(base.at[s], s_sc.at[s], in_sem.at[s]) for s in range(seqs)]
    for c in loads:
        c.start()
    fl = floor[...]
    count = acc[...]
    f, k = [], []
    for j in range(props):
        live = j < count
        fj = fl + (1.0 - fl) * jax.nn.sigmoid(prev_forget[j].astype(F32))
        f.append(jnp.where(live, fj, 1.0))
        k.append(jnp.where(live, 1.0 - fj, 0.0))
    tail = jnp.ones_like(f[0])
    for j in reversed(range(props)):
        bj = k[j] * tail
        for h in range(heads):
            at = (h * props + j) * seqs
            b_sc[at : at + seqs, :] = bj[:, h * HEAD_DIM : (h + 1) * HEAD_DIM]
        tail = tail * f[j]
    for h in range(heads):
        cols = slice(h * HEAD_DIM, (h + 1) * HEAD_DIM)
        a_sc[h] = tail[:, cols].T
    stores = []
    for s in range(seqs):
        loads[s].wait()
        for h in range(heads):
            cols = slice(h * HEAD_DIM, (h + 1) * HEAD_DIM)
            b = b_sc[pl.ds(h * props * seqs + s, props, stride=seqs), :]
            hi = b.astype(BF16)
            lo = (b - hi.astype(F32)).astype(BF16)
            v = prev_input[s, :, cols]
            dims = (((0,), (0,)), ((), ()))
            add = lax.dot_general(hi, v, dims, preferred_element_type=F32) + lax.dot_general(
                lo, v, dims, preferred_element_type=F32
            )
            new = a_sc[h, :, s : s + 1] * s_sc[s, h] + add
            s_sc[s, h] = new
            low[s, h] = new.astype(BF16)
        c = pltpu.make_async_copy(s_sc.at[s], taken.at[s], out_sem.at[s])
        c.start()
        stores.append(c)
    for c in stores:
        c.wait()


def heads_kernel(
    n_kv, seqs, props, heads, x, gain, wq, wf, wi, wg, floor, head_gain, low, out,
    w_sc, s_sc, n_sc, q_sc, o_sc, w_sem, s_sem,
):
    rows = seqs * props
    loads = [pltpu.make_async_copy(w, w_sc.at[i], w_sem.at[i]) for i, w in enumerate((wf, wq, wi, wg))]
    for c in loads:
        c.start()
    s_load = pltpu.make_async_copy(low, s_sc, s_sem)
    s_load.start()
    width = x.shape[2]
    total = jnp.zeros((rows, 1), F32)
    for i in range(n_kv):
        xi = x[i].astype(F32)
        total = total + jnp.sum(xi * xi, axis=1, keepdims=True)
    scale = lax.rsqrt(total / (n_kv * width) + 1e-06)
    for i in range(n_kv):
        c = slice(i * width, (i + 1) * width)
        n_sc[:, c] = (x[i].astype(F32) * scale * gain[:, c]).astype(BF16)

    def project(i):
        loads[i].wait()
        y = jnp.dot(n_sc[...], w_sc[i], preferred_element_type=F32).astype(BF16).astype(F32)
        return [y[t * seqs : (t + 1) * seqs, :] for t in range(props)]

    fl = floor[...]
    f = [fl + (1.0 - fl) * jax.nn.sigmoid(y) for y in project(0)]
    q = [y * jax.nn.sigmoid(y) for y in project(1)]
    decay = jnp.ones_like(f[0])
    for t in range(props):
        decay = decay * f[t]
        qt = q[t] * decay
        for h in range(heads):
            at = (h * props + t) * seqs
            q_sc[at : at + seqs, :] = qt[:, h * HEAD_DIM : (h + 1) * HEAD_DIM]
    v = project(2)
    s_load.wait()
    for s in range(seqs):
        for h in range(heads):
            each = pl.ds(h * props * seqs + s, props, stride=seqs)
            lhs = q_sc[each, :].astype(BF16)
            o_sc[each, :] = jnp.dot(lhs, s_sc[s, h], preferred_element_type=F32)
    g = project(3)
    for t in range(props):
        parts = []
        for h in range(heads):
            cols = slice(h * HEAD_DIM, (h + 1) * HEAD_DIM)
            at = (h * props + t) * seqs
            o = o_sc[at : at + seqs, :]
            reach = q[t][:, cols]
            for i in reversed(range(t + 1)):
                score = jnp.sum(reach * (1.0 - f[i][:, cols]), axis=1, keepdims=True)
                o = o + score * v[i][:, cols]
                reach = reach * f[i][:, cols]
            norm = lax.rsqrt(jnp.mean(o * o, axis=1, keepdims=True) + 1e-05)
            gate = g[t][:, cols]
            parts.append(o * norm * head_gain[...] * (gate * jax.nn.sigmoid(gate)))
        out[t * seqs : (t + 1) * seqs, :] = jnp.concatenate(parts, axis=1).astype(BF16)


def out_kernel(n_tp, r, x, w, out):
    own = x.shape[2]
    total = jnp.dot(x[0], w[:own, :], preferred_element_type=F32)
    for i in range(1, n_tp):
        total = total + jnp.dot(x[i], w[i * own : (i + 1) * own, :], preferred_element_type=F32)
    width = total.shape[1] // r
    for i in range(r):
        out[i] = total[:, i * width : (i + 1) * width].astype(BF16)


def shards(
    n_kv, n_tp, hidden, norm_gain, w_query, w_forget, w_input, w_outgate, w_out, floor, head_gain,
    base_state, prev_forget, prev_input, accepted,
):
    r = n_kv // n_tp
    all_seqs, props, feats = hidden.shape
    seqs = all_seqs // n_kv
    rows = seqs * props
    heads = w_query.shape[1] // HEAD_DIM
    own = heads * HEAD_DIM
    tp = lax.axis_index("tp")
    vmem, anym = pl.BlockSpec(memory_space=pltpu.VMEM), pl.BlockSpec(memory_space=pl.ANY)

    mine = lax.dynamic_slice_in_dim(hidden, tp * (r * seqs), r * seqs, 0)
    mine = mine.reshape(r, seqs, props, feats).transpose(0, 2, 1, 3).reshape(r, rows, feats)
    pieces = exchange(mine, n_kv, n_tp)

    floor_row = floor.reshape(1, own)
    state_shape = base_state.shape
    taken_state, low = pl.pallas_call(
        functools.partial(state_kernel, seqs, props, heads),
        out_shape=(jax.ShapeDtypeStruct(state_shape, F32), jax.ShapeDtypeStruct(state_shape, BF16)),
        in_specs=[vmem, vmem, vmem, vmem, anym],
        out_specs=(anym, vmem),
        scratch_shapes=[
            pltpu.VMEM((heads, HEAD_DIM, seqs), F32),
            pltpu.VMEM((heads * rows, HEAD_DIM), F32),
            pltpu.VMEM(state_shape, F32),
            pltpu.SemaphoreType.DMA((seqs,)),
            pltpu.SemaphoreType.DMA((seqs,)),
        ],
        cost_estimate=pl.CostEstimate(flops=200_000_000, bytes_accessed=6_000_000, transcendentals=0),
        name="state",
    )(accepted.reshape(seqs, 1), floor_row, prev_forget.transpose(1, 0, 2), prev_input, base_state)

    w_part = lax.dynamic_slice_in_dim(w_out, tp * (r * feats), r * feats, 1)
    x = lax.all_gather(pieces, "tp", axis=0, tiled=True)

    mixed_heads = pl.pallas_call(
        functools.partial(heads_kernel, n_kv, seqs, props, heads),
        out_shape=jax.ShapeDtypeStruct((rows, own), BF16),
        in_specs=[vmem, vmem, anym, anym, anym, anym, vmem, vmem, anym],
        out_specs=vmem,
        scratch_shapes=[
            pltpu.VMEM((4, n_kv * feats, own), BF16),
            pltpu.VMEM(state_shape, BF16),
            pltpu.VMEM((rows, n_kv * feats), BF16),
            pltpu.VMEM((heads * rows, HEAD_DIM), F32),
            pltpu.VMEM((heads * rows, HEAD_DIM), F32),
            pltpu.SemaphoreType.DMA((4,)),
            pltpu.SemaphoreType.DMA,
        ],
        cost_estimate=pl.CostEstimate(flops=300_000_000, bytes_accessed=6_000_000, transcendentals=0),
        name="heads",
    )(x, norm_gain.reshape(1, -1), w_query, w_forget, w_input, w_outgate, floor_row, head_gain.reshape(1, -1), low)

    whole = lax.all_gather(mixed_heads, "tp", axis=0)
    finished = pl.pallas_call(
        functools.partial(out_kernel, n_tp, r),
        out_shape=jax.ShapeDtypeStruct((r, rows, feats), BF16),
        in_specs=[vmem, vmem],
        out_specs=vmem,
        name="out",
    )(whole, w_part)
    back = exchange(finished, n_kv, n_tp)
    mixed = lax.all_gather(back, "tp", axis=0, tiled=True)
    mixed = mixed.reshape(n_kv, props, seqs, feats).transpose(0, 2, 1, 3).reshape(all_seqs, props, feats)
    return (mixed, taken_state)


def solution(mesh):
    placed = (
        P(None, None, "kv"),
        P(),
        P(None, "tp"),
        P(None, "tp"),
        P(None, "tp"),
        P(None, "tp"),
        P(),
        P("tp"),
        P(),
        P("kv", "tp", None, None),
        P("kv", None, "tp"),
        P("kv", None, "tp"),
        P("kv"),
    )
    return jax.shard_map(
        functools.partial(shards, mesh.shape["kv"], mesh.shape["tp"]),
        mesh=mesh,
        in_specs=placed,
        out_specs=(P(None, None, "kv"), P("kv", "tp", None, None)),
        check_vma=False,
    )
```

```python
import functools

import jax
import jax.numpy as jnp
from jax import lax
from jax.experimental import pallas as pl
from jax.experimental.pallas import tpu as pltpu
from jax.sharding import PartitionSpec as P

HEAD_DIM = 128
F32 = jnp.float32
BF16 = jnp.bfloat16


def state_kernel(seqs, props, heads, acc, floor, prev_forget, prev_input, base, taken, low, a_sc, b_sc, v_sc, s_sc, in_sem, out_sem):
    loads = [pltpu.make_async_copy(base.at[s], s_sc.at[s], in_sem.at[s]) for s in range(seqs)]
    for c in loads:
        c.start()
    fl = floor[...]
    row = lax.broadcasted_iota(jnp.int32, (seqs, seqs), 0)
    col = lax.broadcasted_iota(jnp.int32, (seqs, seqs), 1)
    count = jnp.sum(jnp.where(row == col, acc[...], 0), axis=1, keepdims=True)
    f, k = [], []
    for j in range(props):
        live = j < count
        fj = fl + (1.0 - fl) * jax.nn.sigmoid(prev_forget[j].astype(F32))
        f.append(jnp.where(live, fj, 1.0))
        k.append(jnp.where(live, 1.0 - fj, 0.0))
    tail = jnp.ones_like(f[0])
    b = [None] * props
    for j in reversed(range(props)):
        b[j] = k[j] * tail
        tail = tail * f[j]
    b = jnp.concatenate(b, axis=0)
    hi = b.astype(BF16).astype(F32)
    both = jnp.concatenate([hi, b - hi], axis=0)
    v = jnp.concatenate([prev_input[j].astype(F32) for j in range(props)] * 2, axis=0)
    owner = lax.broadcasted_iota(jnp.int32, (2 * props * seqs, HEAD_DIM), 0) % seqs
    for h in range(heads):
        cols = slice(h * HEAD_DIM, (h + 1) * HEAD_DIM)
        a_sc[h] = tail[:, cols].T
        b_sc[h] = both[:, cols].T.astype(BF16)
        v_sc[h] = v[:, cols]
    stores = []
    for s in range(seqs):
        loads[s].wait()
        for h in range(heads):
            own_v = jnp.where(owner == s, v_sc[h], 0.0).astype(BF16)
            add = jnp.dot(b_sc[h], own_v, preferred_element_type=F32)
            new = a_sc[h, :, s : s + 1] * s_sc[s, h] + add
            s_sc[s, h] = new
            low[s, h] = new.astype(BF16)
        c = pltpu.make_async_copy(s_sc.at[s], taken.at[s], out_sem.at[s])
        c.start()
        stores.append(c)
    for c in stores:
        c.wait()


def heads_kernel(
    n_kv, seqs, props, heads, x, gain, wq, wf, wi, wg, floor, head_gain, low, out,
    w_sc, s_sc, n_sc, q_sc, o_sc, w_sem, s_sem,
):
    rows = seqs * props
    loads = [pltpu.make_async_copy(w, w_sc.at[i], w_sem.at[i]) for i, w in enumerate((wf, wq, wi, wg))]
    for c in loads:
        c.start()
    s_load = pltpu.make_async_copy(low, s_sc, s_sem)
    s_load.start()
    width = x.shape[2]
    total = jnp.zeros((rows, 1), F32)
    for i in range(n_kv):
        xi = x[i].astype(F32)
        total = total + jnp.sum(xi * xi, axis=1, keepdims=True)
    scale = lax.rsqrt(total / (n_kv * width) + 1e-06)
    for i in range(n_kv):
        c = slice(i * width, (i + 1) * width)
        n_sc[:, c] = (x[i].astype(F32) * scale * gain[:, c]).astype(BF16)

    def project(i):
        loads[i].wait()
        y = jnp.dot(n_sc[...], w_sc[i], preferred_element_type=F32).astype(BF16).astype(F32)
        return [y[t * seqs : (t + 1) * seqs, :] for t in range(props)]

    fl = floor[...]
    f = [fl + (1.0 - fl) * jax.nn.sigmoid(y) for y in project(0)]
    q = [y * jax.nn.sigmoid(y) for y in project(1)]
    decay = jnp.ones_like(f[0])
    for t in range(props):
        decay = decay * f[t]
        qt = q[t] * decay
        for h in range(heads):
            at = (h * props + t) * seqs
            q_sc[at : at + seqs, :] = qt[:, h * HEAD_DIM : (h + 1) * HEAD_DIM]
    v = project(2)
    s_load.wait()
    for s in range(seqs):
        for h in range(heads):
            each = pl.ds(h * props * seqs + s, props, stride=seqs)
            lhs = q_sc[each, :].astype(BF16)
            o_sc[each, :] = jnp.dot(lhs, s_sc[s, h], preferred_element_type=F32)
    g = project(3)
    for t in range(props):
        parts = []
        for h in range(heads):
            cols = slice(h * HEAD_DIM, (h + 1) * HEAD_DIM)
            at = (h * props + t) * seqs
            o = o_sc[at : at + seqs, :]
            reach = q[t][:, cols]
            for i in reversed(range(t + 1)):
                score = jnp.sum(reach * (1.0 - f[i][:, cols]), axis=1, keepdims=True)
                o = o + score * v[i][:, cols]
                reach = reach * f[i][:, cols]
            norm = lax.rsqrt(jnp.mean(o * o, axis=1, keepdims=True) + 1e-05)
            gate = g[t][:, cols]
            parts.append(o * norm * head_gain[...] * (gate * jax.nn.sigmoid(gate)))
        out[t * seqs : (t + 1) * seqs, :] = jnp.concatenate(parts, axis=1).astype(BF16)


def out_kernel(n_tp, n_kv, x, w, out):
    own, feats = x.shape[2], out.shape[2]
    block = max(feats, 2 * HEAD_DIM)
    for b in range(n_kv * feats // block):
        cols = slice(b * block, (b + 1) * block)
        total = jnp.dot(x[0], w[:own, cols], preferred_element_type=F32)
        for i in range(1, n_tp):
            total = total + jnp.dot(x[i], w[i * own : (i + 1) * own, cols], preferred_element_type=F32)
        for i in range(block // feats):
            out[b * (block // feats) + i] = total[:, i * feats : (i + 1) * feats].astype(BF16)


def shards(
    n_kv, n_tp, hidden, norm_gain, w_query, w_forget, w_input, w_outgate, w_out, floor, head_gain,
    base_state, prev_forget, prev_input, accepted,
):
    all_seqs, props, feats = hidden.shape
    seqs = all_seqs // n_kv
    rows = seqs * props
    heads = w_query.shape[1] // HEAD_DIM
    own = heads * HEAD_DIM
    vmem, anym, hbm = (pl.BlockSpec(memory_space=m) for m in (pltpu.VMEM, pl.ANY, pltpu.HBM))

    arrived = lax.all_to_all(hidden, "kv", split_axis=0, concat_axis=0, tiled=True)
    x = arrived.reshape(n_kv, seqs, props, feats).transpose(0, 2, 1, 3).reshape(n_kv, rows, feats)

    floor_row = floor.reshape(1, own)
    state_shape = base_state.shape
    taken_state, low = pl.pallas_call(
        functools.partial(state_kernel, seqs, props, heads),
        out_shape=(jax.ShapeDtypeStruct(state_shape, F32), jax.ShapeDtypeStruct(state_shape, BF16)),
        in_specs=[vmem, vmem, vmem, vmem, hbm],
        out_specs=(hbm, vmem),
        scratch_shapes=[
            pltpu.VMEM((heads, HEAD_DIM, seqs), F32),
            pltpu.VMEM((heads, HEAD_DIM, 2 * rows), BF16),
            pltpu.VMEM((heads, 2 * rows, HEAD_DIM), F32),
            pltpu.VMEM(state_shape, F32),
            pltpu.SemaphoreType.DMA((seqs,)),
            pltpu.SemaphoreType.DMA((seqs,)),
        ],
        cost_estimate=pl.CostEstimate(flops=200_000_000, bytes_accessed=6_000_000, transcendentals=0),
        compiler_params=pltpu.CompilerParams(vmem_limit_bytes=16 * 2**20),
        name="state",
    )(
        accepted.reshape(1, seqs), floor_row, prev_forget.transpose(1, 0, 2), prev_input.transpose(1, 0, 2), base_state
    )

    mixed_heads = pl.pallas_call(
        functools.partial(heads_kernel, n_kv, seqs, props, heads),
        out_shape=jax.ShapeDtypeStruct((rows, own), BF16),
        in_specs=[vmem, vmem, anym, anym, hbm, hbm, vmem, vmem, anym],
        out_specs=vmem,
        scratch_shapes=[
            pltpu.VMEM((4, n_kv * feats, own), BF16),
            pltpu.VMEM(state_shape, BF16),
            pltpu.VMEM((rows, n_kv * feats), BF16),
            pltpu.VMEM((heads * rows, HEAD_DIM), F32),
            pltpu.VMEM((heads * rows, HEAD_DIM), F32),
            pltpu.SemaphoreType.DMA((4,)),
            pltpu.SemaphoreType.DMA,
        ],
        cost_estimate=pl.CostEstimate(flops=300_000_000, bytes_accessed=6_000_000, transcendentals=0),
        compiler_params=pltpu.CompilerParams(vmem_limit_bytes=16 * 2**20),
        name="heads",
    )(x, norm_gain.reshape(1, -1), w_query, w_forget, w_input, w_outgate, floor_row, head_gain.reshape(1, -1), low)

    whole = lax.all_gather(mixed_heads, "tp", axis=0)
    finished = pl.pallas_call(
        functools.partial(out_kernel, n_tp, n_kv),
        out_shape=jax.ShapeDtypeStruct((n_kv, rows, feats), BF16),
        in_specs=[vmem, vmem],
        out_specs=vmem,
        compiler_params=pltpu.CompilerParams(vmem_limit_bytes=16 * 2**20),
        name="out",
    )(whole, w_out)
    mixed = lax.all_to_all(finished, "kv", split_axis=0, concat_axis=0, tiled=True)
    mixed = mixed.reshape(n_kv, props, seqs, feats).transpose(0, 2, 1, 3).reshape(all_seqs, props, feats)
    return (mixed, taken_state)


def solution(mesh):
    placed = (
        P(None, None, "kv"),
        P(),
        P(None, "tp"),
        P(None, "tp"),
        P(None, "tp"),
        P(None, "tp"),
        P(),
        P("tp"),
        P(),
        P("kv", "tp", None, None),
        P("kv", None, "tp"),
        P("kv", None, "tp"),
        P("kv"),
    )
    return jax.shard_map(
        functools.partial(shards, mesh.shape["kv"], mesh.shape["tp"]),
        mesh=mesh,
        in_specs=placed,
        out_specs=(P(None, None, "kv"), P("kv", "tp", None, None)),
        check_vma=False,
    )
```

```python
import functools

import jax
import jax.numpy as jnp
from jax import lax
from jax.experimental import pallas as pl
from jax.experimental.pallas import tpu as pltpu
from jax.sharding import PartitionSpec as P

HEAD_DIM = 128
F32 = jnp.float32
BF16 = jnp.bfloat16


def state_kernel(seqs, props, heads, acc, floor, prev_forget, prev_input, base, taken, low, a_sc, b_sc, v_sc, s_sc, in_sem, out_sem):
    loads = [pltpu.make_async_copy(base.at[s], s_sc.at[s], in_sem.at[s]) for s in range(seqs)]
    for c in loads:
        c.start()
    fl = floor[...]
    row = lax.broadcasted_iota(jnp.int32, (seqs, seqs), 0)
    col = lax.broadcasted_iota(jnp.int32, (seqs, seqs), 1)
    count = jnp.sum(jnp.where(row == col, acc[...], 0), axis=1, keepdims=True)
    f, k = [], []
    for j in range(props):
        live = j < count
        fj = fl + (1.0 - fl) * jax.nn.sigmoid(prev_forget[j].astype(F32))
        f.append(jnp.where(live, fj, 1.0))
        k.append(jnp.where(live, 1.0 - fj, 0.0))
    tail = jnp.ones_like(f[0])
    b = [None] * props
    for j in reversed(range(props)):
        b[j] = k[j] * tail
        tail = tail * f[j]
    b = jnp.concatenate(b, axis=0)
    hi = b.astype(BF16).astype(F32)
    both = jnp.concatenate([hi, b - hi], axis=0)
    v = jnp.concatenate([prev_input[j].astype(F32) for j in range(props)] * 2, axis=0)
    owner = lax.broadcasted_iota(jnp.int32, (2 * props * seqs, HEAD_DIM), 0) % seqs
    for h in range(heads):
        cols = slice(h * HEAD_DIM, (h + 1) * HEAD_DIM)
        a_sc[h] = tail[:, cols].T
        b_sc[h] = both[:, cols].T.astype(BF16)
        v_sc[h] = v[:, cols]
    stores = []
    for s in range(seqs):
        loads[s].wait()
        for h in range(heads):
            own_v = jnp.where(owner == s, v_sc[h], 0.0).astype(BF16)
            add = jnp.dot(b_sc[h], own_v, preferred_element_type=F32)
            new = a_sc[h, :, s : s + 1] * s_sc[s, h] + add
            s_sc[s, h] = new
            low[s, h] = new.astype(BF16)
        c = pltpu.make_async_copy(s_sc.at[s], taken.at[s], out_sem.at[s])
        c.start()
        stores.append(c)
    for c in stores:
        c.wait()


def heads_kernel(
    n_kv, seqs, props, heads, x, gain, wq, wf, wi, wg, floor, head_gain, low, out,
    w_sc, s_sc, n_sc, q_sc, o_sc, w_sem, s_sem,
):
    rows = seqs * props
    loads = [pltpu.make_async_copy(w, w_sc.at[i], w_sem.at[i]) for i, w in enumerate((wf, wq, wi, wg))]
    for c in loads:
        c.start()
    s_load = pltpu.make_async_copy(low, s_sc, s_sem)
    s_load.start()
    width = x.shape[2]
    total = jnp.zeros((rows, 1), F32)
    for i in range(n_kv):
        xi = x[i].astype(F32)
        total = total + jnp.sum(xi * xi, axis=1, keepdims=True)
    scale = lax.rsqrt(total / (n_kv * width) + 1e-06)
    for i in range(n_kv):
        c = slice(i * width, (i + 1) * width)
        n_sc[:, c] = (x[i].astype(F32) * scale * gain[:, c]).astype(BF16)

    def project(i):
        loads[i].wait()
        y = jnp.dot(n_sc[...], w_sc[i], preferred_element_type=F32).astype(BF16).astype(F32)
        return [y[t * seqs : (t + 1) * seqs, :] for t in range(props)]

    fl = floor[...]
    f = [fl + (1.0 - fl) * jax.nn.sigmoid(y) for y in project(0)]
    q = [y * jax.nn.sigmoid(y) for y in project(1)]
    decay = jnp.ones_like(f[0])
    for t in range(props):
        decay = decay * f[t]
        qt = q[t] * decay
        for h in range(heads):
            at = (h * props + t) * seqs
            q_sc[at : at + seqs, :] = qt[:, h * HEAD_DIM : (h + 1) * HEAD_DIM]
    v = project(2)
    s_load.wait()
    for s in range(seqs):
        for h in range(heads):
            each = pl.ds(h * props * seqs + s, props, stride=seqs)
            lhs = q_sc[each, :].astype(BF16)
            o_sc[each, :] = jnp.dot(lhs, s_sc[s, h], preferred_element_type=F32)
    g = project(3)
    for t in range(props):
        parts = []
        for h in range(heads):
            cols = slice(h * HEAD_DIM, (h + 1) * HEAD_DIM)
            at = (h * props + t) * seqs
            o = o_sc[at : at + seqs, :]
            reach = q[t][:, cols]
            for i in reversed(range(t + 1)):
                score = jnp.sum(reach * (1.0 - f[i][:, cols]), axis=1, keepdims=True)
                o = o + score * v[i][:, cols]
                reach = reach * f[i][:, cols]
            norm = lax.rsqrt(jnp.mean(o * o, axis=1, keepdims=True) + 1e-05)
            gate = g[t][:, cols]
            parts.append(o * norm * head_gain[...] * (gate * jax.nn.sigmoid(gate)))
        out[t * seqs : (t + 1) * seqs, :] = jnp.concatenate(parts, axis=1).astype(BF16)


def out_kernel(n_tp, n_kv, x, w, out):
    own, feats = x.shape[2], out.shape[2]
    block = max(feats, 2 * HEAD_DIM)
    for b in range(n_kv * feats // block):
        cols = slice(b * block, (b + 1) * block)
        total = jnp.dot(x[0], w[:own, cols], preferred_element_type=F32)
        for i in range(1, n_tp):
            total = total + jnp.dot(x[i], w[i * own : (i + 1) * own, cols], preferred_element_type=F32)
        for i in range(block // feats):
            out[b * (block // feats) + i] = total[:, i * feats : (i + 1) * feats].astype(BF16)


def shards(
    n_kv, n_tp, hidden, norm_gain, w_query, w_forget, w_input, w_outgate, w_out, floor, head_gain,
    base_state, prev_forget, prev_input, accepted,
):
    all_seqs, props, feats = hidden.shape
    seqs = all_seqs // n_kv
    rows = seqs * props
    heads = w_query.shape[1] // HEAD_DIM
    own = heads * HEAD_DIM
    vmem, anym, hbm = (pl.BlockSpec(memory_space=m) for m in (pltpu.VMEM, pl.ANY, pltpu.HBM))

    arrived = lax.all_to_all(hidden, "kv", split_axis=0, concat_axis=0, tiled=True)
    x = arrived.reshape(n_kv, seqs, props, feats).transpose(0, 2, 1, 3).reshape(n_kv, rows, feats)

    base_state, w_input, w_outgate = (pltpu.with_memory_space_constraint(a, pltpu.HBM) for a in (base_state, w_input, w_outgate))
    floor_row = floor.reshape(1, own)
    state_shape = base_state.shape
    taken_state, low = pl.pallas_call(
        functools.partial(state_kernel, seqs, props, heads),
        out_shape=(jax.ShapeDtypeStruct(state_shape, F32), jax.ShapeDtypeStruct(state_shape, BF16)),
        in_specs=[vmem, vmem, vmem, vmem, hbm],
        out_specs=(hbm, vmem),
        scratch_shapes=[
            pltpu.VMEM((heads, HEAD_DIM, seqs), F32),
            pltpu.VMEM((heads, HEAD_DIM, 2 * rows), BF16),
            pltpu.VMEM((heads, 2 * rows, HEAD_DIM), F32),
            pltpu.VMEM(state_shape, F32),
            pltpu.SemaphoreType.DMA((seqs,)),
            pltpu.SemaphoreType.DMA((seqs,)),
        ],
        cost_estimate=pl.CostEstimate(flops=200_000_000, bytes_accessed=6_000_000, transcendentals=0),
        compiler_params=pltpu.CompilerParams(vmem_limit_bytes=16 * 2**20),
        name="state",
    )(
        pltpu.with_memory_space_constraint(accepted.reshape(1, seqs), pltpu.HBM),
        pltpu.with_memory_space_constraint(floor_row, pltpu.HBM), prev_forget.transpose(1, 0, 2), prev_input.transpose(1, 0, 2), base_state
    )

    mixed_heads = pl.pallas_call(
        functools.partial(heads_kernel, n_kv, seqs, props, heads),
        out_shape=jax.ShapeDtypeStruct((rows, own), BF16),
        in_specs=[vmem, vmem, anym, anym, hbm, hbm, vmem, vmem, anym],
        out_specs=vmem,
        scratch_shapes=[
            pltpu.VMEM((4, n_kv * feats, own), BF16),
            pltpu.VMEM(state_shape, BF16),
            pltpu.VMEM((rows, n_kv * feats), BF16),
            pltpu.VMEM((heads * rows, HEAD_DIM), F32),
            pltpu.VMEM((heads * rows, HEAD_DIM), F32),
            pltpu.SemaphoreType.DMA((4,)),
            pltpu.SemaphoreType.DMA,
        ],
        cost_estimate=pl.CostEstimate(flops=300_000_000, bytes_accessed=6_000_000, transcendentals=0),
        compiler_params=pltpu.CompilerParams(vmem_limit_bytes=16 * 2**20),
        name="heads",
    )(x, norm_gain.reshape(1, -1), w_query, w_forget, w_input, w_outgate, floor_row, head_gain.reshape(1, -1), low)

    whole = lax.all_gather(mixed_heads, "tp", axis=0)
    finished = pl.pallas_call(
        functools.partial(out_kernel, n_tp, n_kv),
        out_shape=jax.ShapeDtypeStruct((n_kv, rows, feats), BF16),
        in_specs=[vmem, vmem],
        out_specs=vmem,
        compiler_params=pltpu.CompilerParams(vmem_limit_bytes=16 * 2**20),
        name="out",
    )(whole, w_out)
    mixed = lax.all_to_all(finished, "kv", split_axis=0, concat_axis=0, tiled=True)
    mixed = mixed.reshape(n_kv, props, seqs, feats).transpose(0, 2, 1, 3).reshape(all_seqs, props, feats)
    return (mixed, taken_state)


def solution(mesh):
    placed = (
        P(None, None, "kv"),
        P(),
        P(None, "tp"),
        P(None, "tp"),
        P(None, "tp"),
        P(None, "tp"),
        P(),
        P("tp"),
        P(),
        P("kv", "tp", None, None),
        P("kv", None, "tp"),
        P("kv", None, "tp"),
        P("kv"),
    )
    return jax.shard_map(
        functools.partial(shards, mesh.shape["kv"], mesh.shape["tp"]),
        mesh=mesh,
        in_specs=placed,
        out_specs=(P(None, None, "kv"), P("kv", "tp", None, None)),
        check_vma=False,
    )
```

```python
import functools

import jax
import jax.numpy as jnp
from jax import lax
from jax.experimental import pallas as pl
from jax.experimental.pallas import tpu as pltpu
from jax.sharding import PartitionSpec as P

HEAD_DIM = 128
F32 = jnp.float32
BF16 = jnp.bfloat16


def state_kernel(seqs, props, heads, acc, floor, prev_forget, prev_input, base, taken, low, a_sc, b_sc, v_sc, s_sc, in_sem, out_sem):
    loads = [pltpu.make_async_copy(base.at[s], s_sc.at[s], in_sem.at[s]) for s in range(seqs)]
    for c in loads:
        c.start()
    fl = floor[...]
    row = lax.broadcasted_iota(jnp.int32, (seqs, seqs), 0)
    col = lax.broadcasted_iota(jnp.int32, (seqs, seqs), 1)
    count = jnp.sum(jnp.where(row == col, acc[...], 0), axis=1, keepdims=True)
    f, k = [], []
    for j in range(props):
        live = j < count
        fj = fl + (1.0 - fl) * jax.nn.sigmoid(prev_forget[j].astype(F32))
        f.append(jnp.where(live, fj, 1.0))
        k.append(jnp.where(live, 1.0 - fj, 0.0))
    tail = jnp.ones_like(f[0])
    b = [None] * props
    for j in reversed(range(props)):
        b[j] = k[j] * tail
        tail = tail * f[j]
    b = jnp.concatenate(b, axis=0)
    hi = b.astype(BF16).astype(F32)
    both = jnp.concatenate([hi, b - hi], axis=0)
    v = jnp.concatenate([prev_input[j].astype(F32) for j in range(props)] * 2, axis=0)
    owner = lax.broadcasted_iota(jnp.int32, (2 * props * seqs, HEAD_DIM), 0) % seqs
    for h in range(heads):
        cols = slice(h * HEAD_DIM, (h + 1) * HEAD_DIM)
        a_sc[h] = tail[:, cols].T
        b_sc[h] = both[:, cols].T.astype(BF16)
        v_sc[h] = v[:, cols]
    stores = []
    for s in range(seqs):
        loads[s].wait()
        for h in range(heads):
            own_v = jnp.where(owner == s, v_sc[h], 0.0).astype(BF16)
            add = jnp.dot(b_sc[h], own_v, preferred_element_type=F32)
            new = a_sc[h, :, s : s + 1] * s_sc[s, h] + add
            s_sc[s, h] = new
            low[s, h] = new.astype(BF16)
        c = pltpu.make_async_copy(s_sc.at[s], taken.at[s], out_sem.at[s])
        c.start()
        stores.append(c)
    for c in stores:
        c.wait()


def heads_kernel(
    n_kv, seqs, props, heads, x, gain, wq, wf, wi, wg, floor, head_gain, low, out,
    w_sc, n_sc, q_sc, o_sc, w_sem,
):
    rows = seqs * props
    loads = [pltpu.make_async_copy(w, w_sc.at[i], w_sem.at[i]) for i, w in enumerate((wi, wg))]
    for c in loads:
        c.start()
    width = x.shape[2]
    total = jnp.zeros((rows, 1), F32)
    for i in range(n_kv):
        xi = x[i].astype(F32)
        total = total + jnp.sum(xi * xi, axis=1, keepdims=True)
    scale = lax.rsqrt(total / (n_kv * width) + 1e-06)
    for i in range(n_kv):
        c = slice(i * width, (i + 1) * width)
        n_sc[:, c] = (x[i].astype(F32) * scale * gain[:, c]).astype(BF16)

    def project(w, load=None):
        if load is not None:
            load.wait()
        y = jnp.dot(n_sc[...], w[...], preferred_element_type=F32).astype(BF16).astype(F32)
        return [y[t * seqs : (t + 1) * seqs, :] for t in range(props)]

    fl = floor[...]
    f = [fl + (1.0 - fl) * jax.nn.sigmoid(y) for y in project(wf)]
    q = [y * jax.nn.sigmoid(y) for y in project(wq)]
    decay = jnp.ones_like(f[0])
    for t in range(props):
        decay = decay * f[t]
        qt = q[t] * decay
        for h in range(heads):
            at = (h * props + t) * seqs
            q_sc[at : at + seqs, :] = qt[:, h * HEAD_DIM : (h + 1) * HEAD_DIM]
    v = project(w_sc.at[0], loads[0])
    for s in range(seqs):
        for h in range(heads):
            each = pl.ds(h * props * seqs + s, props, stride=seqs)
            lhs = q_sc[each, :].astype(BF16)
            o_sc[each, :] = jnp.dot(lhs, low[s, h], preferred_element_type=F32)
    g = project(w_sc.at[1], loads[1])
    for t in range(props):
        parts = []
        for h in range(heads):
            cols = slice(h * HEAD_DIM, (h + 1) * HEAD_DIM)
            at = (h * props + t) * seqs
            o = o_sc[at : at + seqs, :]
            reach = q[t][:, cols]
            for i in reversed(range(t + 1)):
                score = jnp.sum(reach * (1.0 - f[i][:, cols]), axis=1, keepdims=True)
                o = o + score * v[i][:, cols]
                reach = reach * f[i][:, cols]
            norm = lax.rsqrt(jnp.mean(o * o, axis=1, keepdims=True) + 1e-05)
            gate = g[t][:, cols]
            parts.append(o * norm * head_gain[...] * (gate * jax.nn.sigmoid(gate)))
        out[t * seqs : (t + 1) * seqs, :] = jnp.concatenate(parts, axis=1).astype(BF16)


def out_kernel(n_tp, n_kv, x, w, out):
    own, feats = x.shape[2], out.shape[2]
    block = max(feats, 2 * HEAD_DIM)
    for b in range(n_kv * feats // block):
        cols = slice(b * block, (b + 1) * block)
        total = jnp.dot(x[0], w[:own, cols], preferred_element_type=F32)
        for i in range(1, n_tp):
            total = total + jnp.dot(x[i], w[i * own : (i + 1) * own, cols], preferred_element_type=F32)
        for i in range(block // feats):
            out[b * (block // feats) + i] = total[:, i * feats : (i + 1) * feats].astype(BF16)


def shards(
    n_kv, n_tp, hidden, norm_gain, w_query, w_forget, w_input, w_outgate, w_out, floor, head_gain,
    base_state, prev_forget, prev_input, accepted,
):
    all_seqs, props, feats = hidden.shape
    seqs = all_seqs // n_kv
    rows = seqs * props
    heads = w_query.shape[1] // HEAD_DIM
    own = heads * HEAD_DIM
    vmem, hbm = (pl.BlockSpec(memory_space=m) for m in (pltpu.VMEM, pltpu.HBM))

    arrived = lax.all_to_all(hidden, "kv", split_axis=0, concat_axis=0, tiled=True)
    x = arrived.reshape(n_kv, seqs, props, feats).transpose(0, 2, 1, 3).reshape(n_kv, rows, feats)

    base_state, w_input, w_outgate = (pltpu.with_memory_space_constraint(a, pltpu.HBM) for a in (base_state, w_input, w_outgate))
    floor_row = floor.reshape(1, own)
    state_shape = base_state.shape
    taken_state, low = pl.pallas_call(
        functools.partial(state_kernel, seqs, props, heads),
        out_shape=(jax.ShapeDtypeStruct(state_shape, F32), jax.ShapeDtypeStruct(state_shape, BF16)),
        in_specs=[vmem, vmem, vmem, vmem, hbm],
        out_specs=(hbm, vmem),
        scratch_shapes=[
            pltpu.VMEM((heads, HEAD_DIM, seqs), F32),
            pltpu.VMEM((heads, HEAD_DIM, 2 * rows), BF16),
            pltpu.VMEM((heads, 2 * rows, HEAD_DIM), F32),
            pltpu.VMEM(state_shape, F32),
            pltpu.SemaphoreType.DMA((seqs,)),
            pltpu.SemaphoreType.DMA((seqs,)),
        ],
        cost_estimate=pl.CostEstimate(flops=200_000_000, bytes_accessed=6_000_000, transcendentals=0),
        compiler_params=pltpu.CompilerParams(vmem_limit_bytes=16 * 2**20),
        name="state",
    )(
        pltpu.with_memory_space_constraint(accepted.reshape(1, seqs), pltpu.HBM),
        pltpu.with_memory_space_constraint(floor_row, pltpu.HBM), prev_forget.transpose(1, 0, 2), prev_input.transpose(1, 0, 2), base_state
    )

    mixed_heads = pl.pallas_call(
        functools.partial(heads_kernel, n_kv, seqs, props, heads),
        out_shape=jax.ShapeDtypeStruct((rows, own), BF16),
        in_specs=[vmem, vmem, vmem, vmem, hbm, hbm, vmem, vmem, vmem],
        out_specs=vmem,
        scratch_shapes=[
            pltpu.VMEM((2, n_kv * feats, own), BF16),
            pltpu.VMEM((rows, n_kv * feats), BF16),
            pltpu.VMEM((heads * rows, HEAD_DIM), F32),
            pltpu.VMEM((heads * rows, HEAD_DIM), F32),
            pltpu.SemaphoreType.DMA((2,)),
        ],
        cost_estimate=pl.CostEstimate(flops=300_000_000, bytes_accessed=6_000_000, transcendentals=0),
        compiler_params=pltpu.CompilerParams(vmem_limit_bytes=16 * 2**20),
        name="heads",
    )(x, norm_gain.reshape(1, -1), w_query, w_forget, w_input, w_outgate, floor_row, head_gain.reshape(1, -1), low)

    whole = lax.all_gather(mixed_heads, "tp", axis=0)
    finished = pl.pallas_call(
        functools.partial(out_kernel, n_tp, n_kv),
        out_shape=jax.ShapeDtypeStruct((n_kv, rows, feats), BF16),
        in_specs=[vmem, vmem],
        out_specs=vmem,
        compiler_params=pltpu.CompilerParams(vmem_limit_bytes=16 * 2**20),
        name="out",
    )(whole, w_out)
    mixed = lax.all_to_all(finished, "kv", split_axis=0, concat_axis=0, tiled=True)
    mixed = mixed.reshape(n_kv, props, seqs, feats).transpose(0, 2, 1, 3).reshape(all_seqs, props, feats)
    return (mixed, taken_state)


def solution(mesh):
    placed = (
        P(None, None, "kv"),
        P(),
        P(None, "tp"),
        P(None, "tp"),
        P(None, "tp"),
        P(None, "tp"),
        P(),
        P("tp"),
        P(),
        P("kv", "tp", None, None),
        P("kv", None, "tp"),
        P("kv", None, "tp"),
        P("kv"),
    )
    return jax.shard_map(
        functools.partial(shards, mesh.shape["kv"], mesh.shape["tp"]),
        mesh=mesh,
        in_specs=placed,
        out_specs=(P(None, None, "kv"), P("kv", "tp", None, None)),
        check_vma=False,
    )
```
